32 devices in a mesh: sp: 8 (over z, y), tp: 4 (over x, core).
Axes of the slice: x: 2, y: 2, z: 4, core: 2. Of those that a mesh axis runs over, the one named last changes fastest.
Arguments:
- grad_out: bfloat16 [2048, 2048], P('sp'), may hold values from -6 to 6
- resid: bfloat16 [2048, 2048], P('sp'), may hold values from -6 to 6
- norm_gain: float32 [2048], replicated, may hold values from 0.1 to 1.9
- routes: int32 [2048, 2], P('sp'), may hold values from 0 to 7, all different within a row; in each aligned block of 256 rows (0 to 255, 256 to 511, ...) at most 96 rows name the same one
- route_weights: float32 [2048, 2], P('sp'), may hold values from 0.05 to 1
- gate_weight: bfloat16 [8, 2048, 1536], P('sp', None, 'tp'), may hold values from -0.375 to 0.375
- up_weight: bfloat16 [8, 2048, 1536], P('sp', None, 'tp'), may hold values from -0.375 to 0.375
- down_weight: bfloat16 [8, 1536, 2048], P('sp', 'tp'), may hold values from -0.15625 to 0.15625
- proj_weight: bfloat16 [2048, 512], P(None, 'tp'), may hold values from -0.25 to 0.25
- conv_sum: bfloat16 [2048, 512], P('sp', 'tp'), may hold values from -6 to 6
- conv_gain: float32 [512], P('tp'), may hold values from 0.1 to 1.9
- conv_taps: float32 [31, 512], P(None, 'tp'), may hold values from -1 to 1
- conv_value: bfloat16 [2048, 512], P('sp', 'tp'), may hold values from -6 to 6
- conv_gate: bfloat16 [2048, 512], P('sp', 'tp'), may hold values from -6 to 6
Outputs:
- gate_weight_grad: bfloat16 [8, 2048, 1536], P('sp', None, 'tp')
- up_weight_grad: bfloat16 [8, 2048, 1536], P('sp', None, 'tp')
- down_weight_grad: bfloat16 [8, 1536, 2048], P('sp', 'tp')
- proj_grad: float32 [2048, 512], P('sp', 'tp')
- value_grad: bfloat16 [2048, 512], P('sp', 'tp')
- gate_input_grad: bfloat16 [2048, 512], P('sp', 'tp')
The draws below stay inside these ranges and needn't reach their ends.
Inputs may be any that keep to these rules, and one draw needn't show every extreme that they name: In each aligned block of 256 tokens no expert is named by more than 96 routes, and in some block one expert is named exactly 96 times; a token's two routes name different experts.
All inputs are finite; a program needn't handle non-finite values.
Results may differ from the reference program's by a relative error of at most 0.028.
Values may be sent and summed in bfloat16 or wider, within the bound.
A program may use at most 128 MiB of HBM per device.

```python
import math
import jax
import jax.numpy as jnp
import numpy as np
from jax import lax

D = 2048
F = 1536
CH = 512
CONV_K = 31
TOK_DEV = 256
GROUP = 128
EXPERTS = 8
CAP = 96
TOKENS = 2048
N_SP = 8
N_TP = 4


def raised(result, rng, source, target, blocks, factor):
    owner, partner = [(jnp.arange(result.shape[axis_at]) // (result.shape[axis_at] // blocks)).reshape([-1 if axis == axis_at else 1 for axis in range(result.ndim)]) for axis_at in (source, target)]
    chosen = jax.random.permutation(rng, blocks)[partner]
    strong = (owner == chosen) | (owner == (partner + blocks // 2) % blocks)
    return jnp.where(strong, factor * result, result)


def block_levels(key, extent, pieces, smallest, high):
    loudness = 1.0
    for dim, parts in pieces:
        heights = jax.random.uniform(jax.random.fold_in(jax.random.fold_in(key, 6), dim), (parts,), jnp.float32, smallest / len(pieces), high / len(pieces))
        loudness = loudness * jnp.repeat(jnp.exp(heights), extent[dim] // parts).reshape((-1,) + (1,) * (len(extent) - 1 - dim))
    return loudness


def deal_out(own_key, own, number, rows, number_of, top, reach, skew):
    order = jax.random.permutation(own_key, number_of)
    crowded, ordinary = shares(number_of, rows * top, reach, skew, True), shares(number_of, rows * top, reach, skew, False)
    places = jnp.arange(number_of)

    def named(lengths, rotation):
        used = int((lengths > 0).sum())
        fixed = max(1, used // 4)
        passed = fixed + (places - fixed + rotation * (used - fixed)) % max(1, number_of - fixed)
        return jnp.zeros((number_of,), jnp.int32).at[order[jnp.where(places < fixed, places, passed)]].set(jnp.asarray(lengths, jnp.int32))

    lengths = jnp.where(number % 4 == 0, named(crowded, number // 4), named(ordinary, number - number // 4 - 1))
    mixed = jax.random.permutation(jax.random.fold_in(own, 3), number_of)
    giver, receiver = mixed[0:number_of // 2 * 2:2], mixed[1:number_of // 2 * 2:2]
    room = jnp.minimum(lengths[giver] - 1, reach - lengths[receiver]) // 2
    room = jnp.where((giver == order[0]) | (receiver == order[0]) | (lengths[receiver] == 0), 0, jnp.maximum(room, 0))
    passed = jax.random.randint(jax.random.fold_in(own, 4), (number_of // 2,), 0, 1 << 20) % (room + 1)
    lengths = lengths.at[giver].add(-passed).at[receiver].add(passed)
    items = jnp.searchsorted(jnp.cumsum(lengths), jnp.arange(rows * top), side="right").astype(jnp.int32)
    grid = items.reshape(top, rows).T
    grid = grid[jax.random.permutation(jax.random.fold_in(own, 1), rows)]
    rotation = jax.random.randint(jax.random.fold_in(own, 2), (rows, 1), 0, top)
    return jnp.take_along_axis(grid, (jnp.arange(top)[None, :] + rotation) % top, axis=1)


def shares(amount, total, limit, lean, full):
    portions = [(1 << 20) // math.isqrt(standing ** lean) + 1 for standing in range(1, amount + 1)]
    largest = limit if full else min(limit, max(-(-total // amount), total * portions[0] // sum(portions)))
    least = 1 if total - largest >= amount - 1 else 0
    holding, spare = [largest] + [least] * (amount - 1), total - largest - least * (amount - 1)
    while spare > 0:
        candidates = [i for i in range(1, amount) if holding[i] < largest] or [i for i in range(1, amount) if holding[i] < limit]
        pool, remaining = sum([portions[i] for i in candidates]), spare
        for i in candidates:
            addition = min(limit - holding[i], max(1, remaining * portions[i] // pool), spare)
            holding[i] = holding[i] + addition
            spare = spare - addition
    return np.array(holding)


def gaussian(key, extent, deviation, bound, shards=(), held_as=jnp.bfloat16):
    values = deviation * jax.random.normal(key, extent, jnp.float32)
    if shards:
        values = values * block_levels(key, extent, shards, -0.22, 0.18)
    return jnp.clip(values, -bound, bound).astype(held_as)


def noise_with(rng, dims, deviation, limit, split, heavy, kind=jnp.bfloat16):
    drawn = deviation * jax.random.normal(rng, dims, jnp.float32)
    if split:
        drawn = drawn * block_levels(rng, dims, split, -0.22, 0.18)
    return jnp.clip(raised(drawn, jax.random.fold_in(rng, 3), *heavy), -limit, limit).astype(kind)


def setup_inputs(seed: int = 0) -> dict:
    streams_of = jax.random.split(jax.random.key(seed), 15)
    grad_out = noise_with(streams_of[0], (TOKENS, D), 1.0, 6.0, ((0, 8),), (0, 1, 8, 2.0))
    resid = gaussian(streams_of[1], (TOKENS, D), 1.0, 6.0, ((0, 8),))
    norm_gain = jnp.clip(1.0 + 0.18 * jax.random.normal(streams_of[2], (D,), jnp.float32), 0.1, 1.9)
    routes_keys = jax.random.split(jax.random.fold_in(streams_of[3], 1), TOKENS // TOK_DEV)
    routes_turns = jax.random.permutation(jax.random.fold_in(streams_of[3], 3), TOKENS // TOK_DEV)
    routes = jax.vmap(lambda own, number: deal_out(jax.random.fold_in(streams_of[3], 2), own, number, TOK_DEV, EXPERTS, 2, CAP, 1))(routes_keys, routes_turns).reshape((TOKENS, 2))
    route_weights = jnp.clip(0.05 + 0.95 * jax.random.uniform(streams_of[4], (TOKENS, 2), jnp.float32) ** block_levels(streams_of[4], (TOKENS, 2), ((0, 8),), -0.2, 0.2), 0.05, 1.0)
    gate_weight = gaussian(streams_of[5], (EXPERTS, D, F), (D // 9) ** -0.5, 0.375, ((0, 8), (2, 4)))
    up_weight = gaussian(streams_of[6], (EXPERTS, D, F), (D // 9) ** -0.5, 0.375, ((0, 8), (2, 4)))
    down_weight = gaussian(streams_of[7], (EXPERTS, F, D), F ** -0.5, 0.15625, ((0, 8), (1, 4)))
    proj_weight = gaussian(streams_of[8], (D, CH), CH ** -0.5, 0.25, ((1, 4),))
    conv_sum = gaussian(streams_of[9], (TOKENS, CH), 1.0, 6.0, ((0, 8), (1, 4)))
    conv_gain = jnp.clip(1.0 + 0.18 * jax.random.normal(streams_of[10], (CH,), jnp.float32), 0.1, 1.9)
    conv_taps = gaussian(streams_of[11], (CONV_K, CH), CONV_K ** -0.5, 1.0, ((1, 4),), jnp.float32)
    conv_value = gaussian(streams_of[12], (TOKENS, CH), 1.0, 6.0, ((0, 8), (1, 4)))
    conv_gate = gaussian(streams_of[13], (TOKENS, CH), 1.0, 6.0, ((0, 8), (1, 4)))
    return dict(grad_out=grad_out, resid=resid, norm_gain=norm_gain, routes=routes, route_weights=route_weights, gate_weight=gate_weight, up_weight=up_weight, down_weight=down_weight, proj_weight=proj_weight, conv_sum=conv_sum, conv_gain=conv_gain, conv_taps=conv_taps, conv_value=conv_value, conv_gate=conv_gate)


CLAMP_LIMIT = 7.0
SLOPE_ALPHA = 1.702

def contract_rows(left_side, right_side):
    return lax.dot_general(left_side, right_side, (((0,), (0,)), ((), ())), preferred_element_type=jnp.float32)

def contract_cols(left_side, right_side):
    return lax.dot_general(left_side, right_side, (((1,), (1,)), ((), ())), preferred_element_type=jnp.float32)

def expert_backward(routed_rows, routed_cots, w_gate, w_up, w_down):
    gate_pre = jnp.dot(routed_rows, w_gate, preferred_element_type=jnp.float32)
    up_pre = jnp.dot(routed_rows, w_up, preferred_element_type=jnp.float32)
    gate_clamped = jnp.minimum(gate_pre, CLAMP_LIMIT)
    up_clamped = jnp.clip(up_pre, -CLAMP_LIMIT, CLAMP_LIMIT)
    sigma = jax.nn.sigmoid(SLOPE_ALPHA * gate_clamped)
    gated = gate_clamped * sigma
    act = ((up_clamped + 1.0) * gated).astype(jnp.bfloat16)
    down_grad = contract_rows(act, routed_cots).astype(jnp.bfloat16)
    act_grad = contract_cols(routed_cots, w_down)
    inside = (up_pre > -CLAMP_LIMIT) & (up_pre < CLAMP_LIMIT)
    up_pre_grad = jnp.where(inside, act_grad * gated, 0.0).astype(jnp.bfloat16)
    slope = sigma + SLOPE_ALPHA * gate_clamped * sigma * (1.0 - sigma)
    gate_pre_grad = jnp.where(gate_pre < CLAMP_LIMIT, act_grad * (up_clamped + 1.0) * slope, 0.0).astype(jnp.bfloat16)
    gate_grad = contract_rows(routed_rows, gate_pre_grad).astype(jnp.bfloat16)
    up_grad = contract_rows(routed_rows, up_pre_grad).astype(jnp.bfloat16)
    partial_value = contract_cols(gate_pre_grad, w_gate) + contract_cols(up_pre_grad, w_up)
    return (gate_grad, up_grad, down_grad, partial_value)

def reference(grad_out, resid, norm_gain, routes, route_weights, gate_weight, up_weight, down_weight, proj_weight, conv_sum, conv_gain, conv_taps, conv_value, conv_gate):
    resid_f = resid.astype(jnp.float32)
    inv_rms = lax.rsqrt(lax.optimization_barrier(jnp.mean(resid_f * resid_f, axis=-1, keepdims=True)) + 1e-06)
    normed = (resid_f * inv_rms * norm_gain).astype(jnp.bfloat16)
    scaled = (route_weights[:, :, None] * grad_out.astype(jnp.float32)[:, None, :]).astype(jnp.bfloat16)
    scaled = scaled.reshape(2 * TOKENS, D)
    route_ids = routes.reshape(N_SP, 2 * TOK_DEV)
    one_hot = (route_ids[:, :, None] == jnp.arange(EXPERTS, dtype=jnp.int32)[None, None, :]).astype(jnp.int32)
    slot_rank = lax.optimization_barrier(jnp.sum(jnp.cumsum(one_hot, axis=1) * one_hot, axis=2)) - 1
    slot_index = route_ids * (N_SP * CAP) + jnp.arange(N_SP, dtype=jnp.int32)[:, None] * CAP + slot_rank
    slot_table = jnp.full((EXPERTS * N_SP * CAP,), 2 * TOKENS, jnp.int32)
    slot_table = slot_table.at[slot_index.reshape(-1)].set(jnp.arange(2 * TOKENS, dtype=jnp.int32))
    slot_table = slot_table.reshape(EXPERTS, N_SP * CAP)
    normed_pad = jnp.concatenate([normed, jnp.zeros((1, D), jnp.bfloat16)], axis=0)
    scaled_pad = jnp.concatenate([scaled, jnp.zeros((1, D), jnp.bfloat16)], axis=0)
    block_width = F // N_TP

    def one_expert(route_store, inputs):
        table_row, w_gate, w_up, w_down = inputs
        routed_rows = normed_pad[table_row // 2]
        routed_cots = scaled_pad[table_row]
        gate_parts, up_parts, down_parts = ([], [], [])
        row_total = jnp.zeros((N_SP * CAP, D), jnp.float32)
        for block_number in range(N_TP):
            first_col = block_number * block_width
            gate_grad, up_grad, down_grad, partial_value = expert_backward(routed_rows, routed_cots, w_gate[:, first_col:first_col + block_width], w_up[:, first_col:first_col + block_width], w_down[first_col:first_col + block_width, :])
            gate_parts.append(gate_grad)
            up_parts.append(up_grad)
            down_parts.append(down_grad)
            rounded = lax.optimization_barrier(partial_value.astype(jnp.bfloat16))
            row_total = row_total + rounded.astype(jnp.float32)
        route_store = route_store.at[table_row].set(row_total.astype(jnp.bfloat16))
        return (route_store, (jnp.concatenate(gate_parts, axis=1), jnp.concatenate(up_parts, axis=1), jnp.concatenate(down_parts, axis=0)))
    route_store = jnp.zeros((2 * TOKENS + 1, D), jnp.bfloat16)
    route_store, (gate_weight_grad, up_weight_grad, down_weight_grad) = lax.scan(one_expert, route_store, (slot_table, gate_weight, up_weight, down_weight))
    normed_grad = route_store[:2 * TOKENS].astype(jnp.float32).reshape(TOKENS, 2, D).sum(axis=1).astype(jnp.bfloat16)
    feature_grad = normed_grad.astype(jnp.float32) * norm_gain
    cubed = inv_rms * inv_rms * inv_rms
    resid_grad = (grad_out.astype(jnp.float32) + inv_rms * feature_grad - resid_f * cubed * lax.optimization_barrier(jnp.mean(resid_f * feature_grad, axis=-1, keepdims=True))).astype(jnp.bfloat16)
    summed = conv_sum.astype(jnp.float32).reshape(TOKENS, CH // GROUP, GROUP)
    centre = summed - lax.optimization_barrier(jnp.mean(summed, axis=-1, keepdims=True))
    inv_std = lax.rsqrt(lax.optimization_barrier(jnp.mean(centre * centre, axis=-1, keepdims=True)) + 1e-05)
    grouped = centre * inv_std
    chan_normed = grouped.reshape(TOKENS, CH)
    pre_act = chan_normed * conv_gain
    sigma_conv = jax.nn.sigmoid(pre_act)
    conv_out = (pre_act * sigma_conv).astype(jnp.bfloat16)
    proj_grad = contract_rows(resid_grad, conv_out)
    out_grad = jnp.dot(resid_grad, proj_weight, preferred_element_type=jnp.float32)
    normal_grad = (out_grad * sigma_conv * (1.0 + pre_act * (1.0 - sigma_conv)) * conv_gain).reshape(TOKENS, CH // GROUP, GROUP)
    sum_grad = inv_std * (normal_grad - lax.optimization_barrier(jnp.mean(normal_grad, axis=-1, keepdims=True)) - grouped * lax.optimization_barrier(jnp.mean(normal_grad * grouped, axis=-1, keepdims=True)))
    sum_grad = sum_grad.reshape(TOKENS, CH)
    extended = jnp.concatenate([sum_grad, jnp.zeros((CONV_K - 1, CH), jnp.float32)], axis=0)
    gated_grad = lax.conv_general_dilated(extended[None], conv_taps[::-1][:, None, :], (1,), ((0, 0),), dimension_numbers=('NWC', 'WIO', 'NWC'), feature_group_count=CH, precision=lax.Precision.HIGHEST)[0]
    sigma_gate = jax.nn.sigmoid(conv_gate.astype(jnp.float32))
    value_grad = (gated_grad * sigma_gate).astype(jnp.bfloat16)
    gate_input_grad = (gated_grad * conv_value.astype(jnp.float32) * sigma_gate * (1.0 - sigma_gate)).astype(jnp.bfloat16)
    return (gate_weight_grad, up_weight_grad, down_weight_grad, proj_grad, value_grad, gate_input_grad)
```

```python
import functools

import jax
import jax.numpy as jnp
from jax import lax
from jax.experimental import pallas as pl
from jax.experimental.pallas import tpu as pltpu
from jax.sharding import PartitionSpec as P

CONV_K = 31
GROUP = 128
MESH = pl.DeviceIdType.MESH


CLAMP_LIMIT = 7.0
SLOPE_ALPHA = 1.702


def passed_along(block, axis, distance):
    devices = range(lax.axis_size(axis))
    route = [(i - distance, i) for i in devices if i - distance in devices]
    return lax.ppermute(block, axis, route)


def rotated(block, axis, distance):
    count = lax.axis_size(axis)
    return lax.ppermute(block, axis, [(i, (i + distance) % count) for i in range(count)])


def tp_places():
    mine = lax.axis_index("tp")
    near = mine + 1 - 2 * (mine % 2)
    far = (mine + 2) % 4
    diag = (near + 2) % 4
    return mine, near, far, diag


def meet(steps, over_sp, near, far):
    s, t = lax.axis_index("sp"), lax.axis_index("tp")
    barrier = pltpu.get_barrier_semaphore()
    pl.semaphore_signal(barrier, inc=1, device_id=(s, near), device_id_type=MESH)
    pl.semaphore_signal(barrier, inc=1, device_id=(s, far), device_id_type=MESH)
    total = 2
    if over_sp:

        def greet(d, carry):
            pl.semaphore_signal(
                barrier, inc=1, device_id=((s + d) % steps, t), device_id_type=MESH
            )
            return carry

        lax.fori_loop(1, steps, greet, 0)
        total += steps - 1
    pl.semaphore_wait(barrier, total)


def spread_kernel(count, steps, over_sp, in_lanes, absolute, *refs):
    sends, outs = refs[:count], refs[count : 2 * count]
    own_sem, a_send, a_recv, b_send, f_send, c_send, near_recv, fwd_recv, far_recv = refs[2 * count :]
    s = lax.axis_index("sp")
    t, near, far, _ = tp_places()
    width = sends[0].shape[-1]

    def place(c, d, q):
        if in_lanes:
            return outs[c].at[d, :, pl.ds(pl.multiple_of(q * width, width), width)]
        return outs[c].at[d, q]

    def source(c, d):
        return sends[c].at[(s + d) % steps if absolute else d]

    def own(c, d):
        return pltpu.make_async_copy(source(c, d), place(c, d, t), own_sem.at[c, d])

    def to_sp(c, d):
        return pltpu.make_async_remote_copy(
            src_ref=source(c, d),
            dst_ref=place(c, d, t),
            send_sem=a_send.at[c, d],
            recv_sem=a_recv.at[c, d],
            device_id=((s + d) % steps, t),
            device_id_type=MESH,
        )

    def to_tp(c, d, q, target, send_sem, recv_sem):
        return pltpu.make_async_remote_copy(
            src_ref=place(c, d, q),
            dst_ref=place(c, d, q),
            send_sem=send_sem.at[c, d],
            recv_sem=recv_sem.at[c, d],
            device_id=(s, target),
            device_id_type=MESH,
        )

    def near_copy(c, d):
        return to_tp(c, d, t, near, b_send, near_recv)

    def far_copy(c, d):
        return to_tp(c, d, t, far, f_send, far_recv)

    def fwd_copy(c, d):
        return to_tp(c, d, far, near, c_send, fwd_recv)

    def loop(first, last, body):
        def step(d, carry):
            for c in range(count):
                body(c, d)
            return carry

        lax.fori_loop(first, last, step, 0)

    meet(steps, over_sp, near, far)
    remote_from = 1 if over_sp else steps
    loop(0, remote_from, lambda c, d: own(c, d).start())
    loop(remote_from, steps, lambda c, d: to_sp(c, d).start())

    def share(c, d):
        far_copy(c, d).start()
        near_copy(c, d).start()

    def forward(c, d):
        far_copy(c, d).wait_recv()
        fwd_copy(c, d).start()

    def share_own(c, d):
        own(c, d).wait()
        share(c, d)

    def share_arrived(c, d):
        to_sp(c, d).wait_recv()
        share(c, d)
        forward(c, d - 1)

    loop(0, remote_from, share_own)
    loop(remote_from, steps, share_arrived)
    loop(steps - 1 if over_sp else 0, steps, forward)

    def finish(c, d):
        near_copy(c, d).wait()
        far_copy(c, d).wait_send()
        fwd_copy(c, d).wait()

    loop(0, steps, finish)
    loop(remote_from, steps, lambda c, d: to_sp(c, d).wait_send())


def spread(sends, over_sp, in_lanes, absolute, collective_id):
    count = len(sends)
    steps, rows, width = sends[0].shape
    tp_count = lax.axis_size("tp")
    shape = (steps, rows, tp_count * width) if in_lanes else (steps, tp_count, rows, width)
    return pl.pallas_call(
        functools.partial(spread_kernel, count, steps, over_sp, in_lanes, absolute),
        out_shape=tuple(jax.ShapeDtypeStruct(shape, x.dtype) for x in sends),
        in_specs=[pl.BlockSpec(memory_space=pltpu.VMEM)] * count,
        out_specs=tuple(pl.BlockSpec(memory_space=pltpu.VMEM) for _ in sends),
        scratch_shapes=[pltpu.SemaphoreType.DMA((count, steps))] * 9,
        compiler_params=pltpu.CompilerParams(
            collective_id=collective_id, has_side_effects=True, vmem_limit_bytes=40 << 20
        ),
    )(*sends)


def combine_kernel(
    steps, part, out, near_in, pair, far_in, total,
    n0_send, n0_recv, n1_send, n1_recv, f_send, f_recv, a_send, a_recv,
):
    s = lax.axis_index("sp")
    t, near, far, diag = tp_places()
    width = out.shape[-1]

    def lanes(q):
        return pl.ds(pl.multiple_of(q * width, width), width)

    def near_copy(d, which, q, send_sem, recv_sem):
        return pltpu.make_async_remote_copy(
            src_ref=part.at[d, :, lanes(q)],
            dst_ref=near_in.at[which, d],
            send_sem=send_sem.at[d],
            recv_sem=recv_sem.at[d],
            device_id=(s, near),
            device_id_type=MESH,
        )

    def for_near(d):
        return near_copy(d, 0, near, n0_send, n0_recv)

    def for_diag(d):
        return near_copy(d, 1, diag, n1_send, n1_recv)

    def far_copy(d):
        return pltpu.make_async_remote_copy(
            src_ref=pair.at[d],
            dst_ref=far_in.at[d],
            send_sem=f_send.at[d],
            recv_sem=f_recv.at[d],
            device_id=(s, far),
            device_id_type=MESH,
        )

    def back(d):
        return pltpu.make_async_remote_copy(
            src_ref=total.at[d],
            dst_ref=out.at[d],
            send_sem=a_send.at[d],
            recv_sem=a_recv.at[d],
            device_id=((s + steps - d) % steps, t),
            device_id_type=MESH,
        )

    def loop(first, last, body):
        def step(d, carry):
            body(d)
            return carry

        lax.fori_loop(first, last, step, 0)

    meet(steps, True, near, far)

    def open_up(d):
        for_diag(d).start()
        for_near(d).start()

    def add_pair(d):
        for_diag(d).wait_recv()
        mine = part[d, :, lanes(far)].astype(jnp.float32)
        pair[d] = (mine + near_in[1, d].astype(jnp.float32)).astype(pair.dtype)
        far_copy(d).start()

    def whole(d):
        for_near(d).wait_recv()
        far_copy(d).wait_recv()
        mine = part[d, :, lanes(t)].astype(jnp.float32)
        both = mine + near_in[0, d].astype(jnp.float32)
        return (both + far_in[d].astype(jnp.float32)).astype(out.dtype)

    def send_back(d):
        total[d] = whole(d)
        back(d).start()

    loop(1, steps, open_up)
    open_up(0)
    add_pair(1)

    def middle(d):
        add_pair(d)
        send_back(d - 1)

    loop(2, steps, middle)
    add_pair(0)
    send_back(steps - 1)
    out[0] = whole(0)

    def finish(d):
        for_near(d).wait_send()
        for_diag(d).wait_send()
        far_copy(d).wait_send()

    loop(0, steps, finish)
    loop(1, steps, lambda d: back(d).wait())


def combine(part, collective_id):
    steps, rows, all_width = part.shape
    width = all_width // lax.axis_size("tp")
    block = (steps, rows, width)
    return pl.pallas_call(
        functools.partial(combine_kernel, steps),
        out_shape=jax.ShapeDtypeStruct(block, part.dtype),
        in_specs=[pl.BlockSpec(memory_space=pltpu.VMEM)],
        out_specs=pl.BlockSpec(memory_space=pltpu.VMEM),
        scratch_shapes=[
            pltpu.VMEM((2,) + block, part.dtype),
            pltpu.VMEM(block, part.dtype),
            pltpu.VMEM(block, part.dtype),
            pltpu.VMEM(block, part.dtype),
        ]
        + [pltpu.SemaphoreType.DMA((steps,))] * 8,
        compiler_params=pltpu.CompilerParams(
            collective_id=collective_id, has_side_effects=True, vmem_limit_bytes=40 << 20
        ),
    )(part)


def contract_rows(left_side, right_side):
    return lax.dot_general(
        left_side, right_side, (((0,), (0,)), ((), ())), preferred_element_type=jnp.float32
    )


def contract_cols(left_side, right_side):
    return lax.dot_general(
        left_side, right_side, (((1,), (1,)), ((), ())), preferred_element_type=jnp.float32
    )


def expert_backward(routed_rows, routed_cots, w_gate, w_up, w_down):
    gate_pre = jnp.dot(routed_rows, w_gate, preferred_element_type=jnp.float32)
    up_pre = jnp.dot(routed_rows, w_up, preferred_element_type=jnp.float32)
    gate_clamped = jnp.minimum(gate_pre, CLAMP_LIMIT)
    up_clamped = jnp.clip(up_pre, -CLAMP_LIMIT, CLAMP_LIMIT)
    sigma = jax.nn.sigmoid(SLOPE_ALPHA * gate_clamped)
    gated = gate_clamped * sigma
    act = ((up_clamped + 1.0) * gated).astype(jnp.bfloat16)
    down_grad = contract_rows(act, routed_cots).astype(jnp.bfloat16)
    act_grad = contract_cols(routed_cots, w_down)
    inside = (up_pre > -CLAMP_LIMIT) & (up_pre < CLAMP_LIMIT)
    up_pre_grad = jnp.where(inside, act_grad * gated, 0.0).astype(jnp.bfloat16)
    slope = sigma + SLOPE_ALPHA * gate_clamped * sigma * (1.0 - sigma)
    gate_pre_grad = jnp.where(
        gate_pre < CLAMP_LIMIT, act_grad * (up_clamped + 1.0) * slope, 0.0
    ).astype(jnp.bfloat16)
    gate_grad = contract_rows(routed_rows, gate_pre_grad).astype(jnp.bfloat16)
    up_grad = contract_rows(routed_rows, up_pre_grad).astype(jnp.bfloat16)
    partial_value = contract_cols(gate_pre_grad, w_gate) + contract_cols(up_pre_grad, w_up)
    return (gate_grad, up_grad, down_grad, partial_value)


def local(
    grad_out,
    resid,
    norm_gain,
    routes,
    route_weights,
    gate_weight,
    up_weight,
    down_weight,
    proj_weight,
    conv_sum,
    conv_gain,
    conv_taps,
    conv_value,
    conv_gate,
):
    tok_rows, model_width = resid.shape
    sp_count = lax.axis_size("sp")
    tp_count = lax.axis_size("tp")
    capacity = 3 * tok_rows // sp_count
    col_count = model_width // tp_count
    resid_f = resid.astype(jnp.float32)
    inv_rms = lax.rsqrt(jnp.mean(resid_f * resid_f, axis=-1, keepdims=True) + 1e-06)
    normed = (resid_f * inv_rms * norm_gain).astype(jnp.bfloat16)
    my_sp = lax.axis_index("sp")
    away = (routes - my_sp) % sp_count
    steps_away = jnp.arange(sp_count, dtype=jnp.int32)
    named = away[:, :, None] == steps_away[None, None, :]
    chosen = jnp.any(named, axis=1)
    weight_of = jnp.sum(jnp.where(named, route_weights[:, :, None], 0.0), axis=1)
    token_ids = jnp.arange(tok_rows, dtype=jnp.int32)
    earlier = (token_ids[None, :] < token_ids[:, None]).astype(jnp.bfloat16)
    rank = jnp.dot(earlier, chosen.astype(jnp.bfloat16), preferred_element_type=jnp.float32)
    rank = jnp.where(chosen, rank, -1.0).astype(jnp.int32)
    slots = jnp.arange(capacity, dtype=jnp.int32)
    held = rank.T[:, None, :] == slots[None, :, None]
    slot_weight = jnp.sum(jnp.where(held, weight_of.T[:, None, :], 0.0), axis=2)
    pick = held.astype(jnp.bfloat16).reshape(sp_count * capacity, tok_rows)
    first_col = lax.axis_index("tp") * col_count
    normed_part = lax.dynamic_slice_in_dim(normed, first_col, col_count, 1)
    cots_part = lax.dynamic_slice_in_dim(grad_out, first_col, col_count, 1)
    send_rows = jnp.dot(pick, normed_part, preferred_element_type=jnp.float32).astype(jnp.bfloat16)
    send_cots = jnp.dot(pick, cots_part, preferred_element_type=jnp.float32)
    send_cots = (send_cots * slot_weight.reshape(-1, 1)).astype(jnp.bfloat16)
    routed_rows, routed_cots = spread(
        (
            send_rows.reshape(sp_count, capacity, col_count),
            send_cots.reshape(sp_count, capacity, col_count),
        ),
        True,
        True,
        False,
        0,
    )
    routed_rows = routed_rows.reshape(sp_count * capacity, model_width)
    routed_cots = routed_cots.reshape(sp_count * capacity, model_width)
    gate_grad, up_grad, down_grad, partial_value = expert_backward(
        routed_rows, routed_cots, gate_weight[0], up_weight[0], down_weight[0]
    )
    returned = combine(
        partial_value.reshape(sp_count, capacity, model_width).astype(jnp.bfloat16), 1
    ).reshape(sp_count * capacity, col_count)
    normed_part_grad = contract_rows(pick, returned).astype(jnp.bfloat16)
    chunks = 4
    (normed_grad,) = spread(
        (normed_part_grad.reshape(chunks, tok_rows // chunks, col_count),), False, True, False, 2
    )
    normed_grad = normed_grad.reshape(tok_rows, model_width)
    feature_grad = normed_grad.astype(jnp.float32) * norm_gain
    cubed = inv_rms * inv_rms * inv_rms
    resid_grad = (
        grad_out.astype(jnp.float32)
        + inv_rms * feature_grad
        - resid_f * cubed * jnp.mean(resid_f * feature_grad, axis=-1, keepdims=True)
    ).astype(jnp.bfloat16)
    channels = conv_sum.shape[1]
    summed = conv_sum.astype(jnp.float32).reshape(tok_rows, channels // GROUP, GROUP)
    centre = summed - jnp.mean(summed, axis=-1, keepdims=True)
    inv_std = lax.rsqrt(jnp.mean(centre * centre, axis=-1, keepdims=True) + 1e-05)
    grouped = centre * inv_std
    chan_normed = grouped.reshape(tok_rows, channels)
    pre_act = chan_normed * conv_gain
    sigma_conv = jax.nn.sigmoid(pre_act)
    conv_out = (pre_act * sigma_conv).astype(jnp.bfloat16)
    all_out, reach = conv_out, 1
    while reach < sp_count:
        more = min(reach, sp_count - reach)
        all_out = jnp.concatenate([all_out, rotated(all_out[: more * tok_rows], "sp", reach)])
        reach += more
    share = tok_rows // tp_count
    tokens_part = lax.dynamic_slice_in_dim(resid_grad, lax.axis_index("tp") * share, share, 0)
    by_feature = tokens_part.reshape(share, sp_count, model_width // sp_count).transpose(1, 0, 2)
    (feature_cols,) = spread((by_feature,), True, False, True, 3)
    proj_grad = contract_rows(
        feature_cols.reshape(sp_count * tok_rows, model_width // sp_count), all_out
    )
    out_grad = jnp.dot(resid_grad, proj_weight, preferred_element_type=jnp.float32)
    normal_grad = (
        out_grad * sigma_conv * (1.0 + pre_act * (1.0 - sigma_conv)) * conv_gain
    ).reshape(tok_rows, channels // GROUP, GROUP)
    sum_grad = inv_std * (
        normal_grad
        - jnp.mean(normal_grad, axis=-1, keepdims=True)
        - grouped * jnp.mean(normal_grad * grouped, axis=-1, keepdims=True)
    )
    sum_grad = sum_grad.reshape(tok_rows, channels)
    following = passed_along(sum_grad[: CONV_K - 1], "sp", -1)
    extended = jnp.concatenate([sum_grad, following], axis=0)
    gated_grad = lax.conv_general_dilated(
        extended[None],
        conv_taps[::-1][:, None, :],
        (1,),
        ((0, 0),),
        dimension_numbers=("NWC", "WIO", "NWC"),
        feature_group_count=channels,
        precision=lax.Precision.HIGHEST,
    )[0]
    sigma_gate = jax.nn.sigmoid(conv_gate.astype(jnp.float32))
    value_grad = (gated_grad * sigma_gate).astype(jnp.bfloat16)
    gate_input_grad = (
        gated_grad * conv_value.astype(jnp.float32) * sigma_gate * (1.0 - sigma_gate)
    ).astype(jnp.bfloat16)
    return (gate_grad[None], up_grad[None], down_grad[None], proj_grad, value_grad, gate_input_grad)


def solution(mesh):
    in_specs = (
        P("sp", None),
        P("sp", None),
        P(),
        P("sp", None),
        P("sp", None),
        P("sp", None, "tp"),
        P("sp", None, "tp"),
        P("sp", "tp", None),
        P(None, "tp"),
        P("sp", "tp"),
        P("tp"),
        P(None, "tp"),
        P("sp", "tp"),
        P("sp", "tp"),
    )
    out_specs = (
        P("sp", None, "tp"),
        P("sp", None, "tp"),
        P("sp", "tp", None),
        P("sp", "tp"),
        P("sp", "tp"),
        P("sp", "tp"),
    )
    return jax.shard_map(local, mesh=mesh, in_specs=in_specs, out_specs=out_specs, check_vma=False)
```

```python
import functools

import jax
import jax.numpy as jnp
from jax import lax
from jax.experimental import pallas as pl
from jax.experimental.pallas import tpu as pltpu
from jax.sharding import PartitionSpec as P

CONV_K = 31
GROUP = 128
MESH = pl.DeviceIdType.MESH


CLAMP_LIMIT = 7.0
SLOPE_ALPHA = 1.702


def passed_along(block, axis, distance):
    devices = range(lax.axis_size(axis))
    route = [(i - distance, i) for i in devices if i - distance in devices]
    return lax.ppermute(block, axis, route)


def tp_places():
    mine = lax.axis_index("tp")
    near = mine + 1 - 2 * (mine % 2)
    far = (mine + 2) % 4
    diag = (near + 2) % 4
    return mine, near, far, diag


def meet(steps, over_sp, near, far):
    s, t = lax.axis_index("sp"), lax.axis_index("tp")
    barrier = pltpu.get_barrier_semaphore()
    pl.semaphore_signal(barrier, inc=1, device_id=(s, near), device_id_type=MESH)
    pl.semaphore_signal(barrier, inc=1, device_id=(s, far), device_id_type=MESH)
    total = 2
    if over_sp:

        def greet(d, carry):
            pl.semaphore_signal(
                barrier, inc=1, device_id=((s + d) % steps, t), device_id_type=MESH
            )
            return carry

        lax.fori_loop(1, steps, greet, 0)
        total += steps - 1
    pl.semaphore_wait(barrier, total)


def crossing_first(steps, k):
    return steps // 2 + ((k + 1) // 2) * (2 * (k % 2) - 1)


def looped(first, last, body):
    def step(k, carry):
        body(k)
        return carry

    lax.fori_loop(first, last, step, 0)


def spread_kernel(count, steps, over_sp, in_lanes, absolute, beside, sp_count, *refs):
    refs = list(refs)
    sends, refs = refs[:count], refs[count:]
    fulls, refs = (refs[:count], refs[count:]) if over_sp else (None, refs)
    side, refs = (refs[0], refs[1:]) if beside else (None, refs)
    outs, refs = refs[:count], refs[count:]
    side_out, refs = (refs[0], refs[1:]) if beside else (None, refs)
    own_sem, a_send, a_recv, b_send, f_send, c_send, near_recv, fwd_recv, far_recv = refs[:9]
    s = lax.axis_index("sp")
    t, near, far, _ = tp_places()
    width = sends[0].shape[-1]

    def place(c, d, q):
        if in_lanes:
            return outs[c].at[d, :, pl.ds(pl.multiple_of(q * width, width), width)]
        return outs[c].at[d, q]

    def source(c, d):
        return sends[c].at[(s + d) % steps if absolute else d]

    def own(c, d):
        if over_sp:
            return pltpu.make_async_copy(fulls[c], outs[c].at[0], own_sem.at[c, 0])
        return pltpu.make_async_copy(source(c, d), place(c, d, t), own_sem.at[c, d])

    def to_sp(c, d):
        return pltpu.make_async_remote_copy(
            src_ref=source(c, d),
            dst_ref=place(c, d, t),
            send_sem=a_send.at[c, d],
            recv_sem=a_recv.at[c, d],
            device_id=((s + d) % steps, t),
            device_id_type=MESH,
        )

    def to_tp(c, d, q, target, send_sem, recv_sem):
        return pltpu.make_async_remote_copy(
            src_ref=place(c, d, q),
            dst_ref=place(c, d, q),
            send_sem=send_sem.at[c, d],
            recv_sem=recv_sem.at[c, d],
            device_id=(s, target),
            device_id_type=MESH,
        )

    def near_copy(c, d):
        return to_tp(c, d, t, near, b_send, near_recv)

    def far_copy(c, d):
        return to_tp(c, d, t, far, f_send, far_recv)

    def fwd_copy(c, d):
        return to_tp(c, d, far, near, c_send, fwd_recv)

    def side_copy(d):
        side_send, side_recv = refs[10:12]
        return pltpu.make_async_remote_copy(
            src_ref=side,
            dst_ref=side_out.at[d],
            send_sem=side_send.at[d],
            recv_sem=side_recv.at[d],
            device_id=((s + d) % sp_count, t),
            device_id_type=MESH,
        )

    def own_side():
        return pltpu.make_async_copy(side, side_out.at[0], refs[9].at[0])

    def share(c, d):
        far_copy(c, d).start()
        near_copy(c, d).start()

    def forward(c, d):
        far_copy(c, d).wait_recv()
        fwd_copy(c, d).start()

    def finish(c, d):
        near_copy(c, d).wait()
        far_copy(c, d).wait_send()
        fwd_copy(c, d).wait()

    def loop(first, last, body):
        def each(k):
            d = crossing_first(steps, k) if over_sp else k
            for c in range(count):
                body(c, d)

        looped(first, last, each)

    meet(sp_count, over_sp or beside, near, far)
    if over_sp:
        loop(0, steps - 1, lambda c, d: to_sp(c, d).start())
        for c in range(count):
            own(c, 0).start()

        def pass_on(k):
            for c in range(count):
                d = crossing_first(steps, k)
                to_sp(c, d).wait_recv()
                share(c, d)

        def pass_on_twice(k):
            pass_on(k)
            for c in range(count):
                forward(c, crossing_first(steps, k - 1))

        pass_on(0)
        looped(1, steps - 1, pass_on_twice)
        loop(steps - 2, steps - 1, forward)
        loop(0, steps - 1, finish)
        loop(0, steps - 1, lambda c, d: to_sp(c, d).wait_send())
        for c in range(count):
            own(c, 0).wait()
    else:
        loop(0, steps, lambda c, d: own(c, d).start())
        if beside:
            looped(0, sp_count - 1, lambda k: side_copy(crossing_first(sp_count, k)).start())
            own_side().start()

        def share_own(c, d):
            own(c, d).wait()
            share(c, d)

        loop(0, steps, share_own)
        loop(0, steps, forward)
        loop(0, steps, finish)
        if beside:
            looped(0, sp_count - 1, lambda k: side_copy(crossing_first(sp_count, k)).wait())
            own_side().wait()


def spread(sends, fulls, side, in_lanes, absolute, collective_id):
    count = len(sends)
    steps, rows, width = sends[0].shape
    tp_count, sp_count = lax.axis_size("tp"), lax.axis_size("sp")
    over_sp, beside = fulls is not None, side is not None
    shape = (steps, rows, tp_count * width) if in_lanes else (steps, tp_count, rows, width)
    out_shape = [jax.ShapeDtypeStruct(shape, x.dtype) for x in sends]
    operands = list(sends) + (list(fulls) if over_sp else []) + ([side] if beside else [])
    scratch = [pltpu.SemaphoreType.DMA((count, steps))] * 9
    if beside:
        out_shape.append(jax.ShapeDtypeStruct((sp_count,) + side.shape, side.dtype))
        scratch += [pltpu.SemaphoreType.DMA((1,))] + [pltpu.SemaphoreType.DMA((sp_count,))] * 2
    return pl.pallas_call(
        functools.partial(
            spread_kernel, count, steps, over_sp, in_lanes, absolute, beside, sp_count
        ),
        out_shape=tuple(out_shape),
        in_specs=[pl.BlockSpec(memory_space=pltpu.VMEM)] * len(operands),
        out_specs=tuple(pl.BlockSpec(memory_space=pltpu.VMEM) for _ in out_shape),
        scratch_shapes=scratch,
        compiler_params=pltpu.CompilerParams(
            collective_id=collective_id, has_side_effects=True, vmem_limit_bytes=40 << 20
        ),
    )(*operands)


def combine_kernel(
    steps, part, out, near_in, pair, far_in, total,
    n0_send, n0_recv, n1_send, n1_recv, f_send, f_recv, a_send, a_recv,
):
    s = lax.axis_index("sp")
    t, near, far, diag = tp_places()
    width = out.shape[-1]

    def lanes(q):
        return pl.ds(pl.multiple_of(q * width, width), width)

    def near_copy(d, which, q, send_sem, recv_sem):
        return pltpu.make_async_remote_copy(
            src_ref=part.at[d, :, lanes(q)],
            dst_ref=near_in.at[which, d],
            send_sem=send_sem.at[d],
            recv_sem=recv_sem.at[d],
            device_id=(s, near),
            device_id_type=MESH,
        )

    def for_near(d):
        return near_copy(d, 0, near, n0_send, n0_recv)

    def for_diag(d):
        return near_copy(d, 1, diag, n1_send, n1_recv)

    def far_copy(d):
        return pltpu.make_async_remote_copy(
            src_ref=pair.at[d],
            dst_ref=far_in.at[d],
            send_sem=f_send.at[d],
            recv_sem=f_recv.at[d],
            device_id=(s, far),
            device_id_type=MESH,
        )

    def back(d):
        return pltpu.make_async_remote_copy(
            src_ref=total.at[d],
            dst_ref=out.at[d],
            send_sem=a_send.at[d],
            recv_sem=a_recv.at[d],
            device_id=((s + steps - d) % steps, t),
            device_id_type=MESH,
        )

    meet(steps, True, near, far)

    def open_up(d):
        for_diag(d).start()
        for_near(d).start()

    def add_pair(d):
        for_diag(d).wait_recv()
        mine = part[d, :, lanes(far)].astype(jnp.float32)
        pair[d] = (mine + near_in[1, d].astype(jnp.float32)).astype(pair.dtype)
        far_copy(d).start()

    def whole(d):
        for_near(d).wait_recv()
        far_copy(d).wait_recv()
        mine = part[d, :, lanes(t)].astype(jnp.float32)
        both = mine + near_in[0, d].astype(jnp.float32)
        return (both + far_in[d].astype(jnp.float32)).astype(out.dtype)

    def send_back(d):
        total[d] = whole(d)
        back(d).start()

    def at(k):
        return crossing_first(steps, k)

    lag = min(3, steps - 1)
    looped(0, steps - 1, lambda k: open_up(at(k)))
    open_up(0)
    looped(0, lag, lambda k: add_pair(at(k)))

    def middle(k):
        add_pair(at(k))
        send_back(at(k - lag))

    looped(lag, steps - 1, middle)
    add_pair(0)
    looped(steps - 1 - lag, steps - 1, lambda k: send_back(at(k)))
    out[0] = whole(0)

    def finish(d):
        for_near(d).wait_send()
        for_diag(d).wait_send()
        far_copy(d).wait_send()

    looped(0, steps, finish)
    looped(1, steps, lambda d: back(d).wait())


def combine(part, collective_id):
    steps, rows, all_width = part.shape
    width = all_width // lax.axis_size("tp")
    block = (steps, rows, width)
    return pl.pallas_call(
        functools.partial(combine_kernel, steps),
        out_shape=jax.ShapeDtypeStruct(block, part.dtype),
        in_specs=[pl.BlockSpec(memory_space=pltpu.VMEM)],
        out_specs=pl.BlockSpec(memory_space=pltpu.VMEM),
        scratch_shapes=[
            pltpu.VMEM((2,) + block, part.dtype),
            pltpu.VMEM(block, part.dtype),
            pltpu.VMEM(block, part.dtype),
            pltpu.VMEM(block, part.dtype),
        ]
        + [pltpu.SemaphoreType.DMA((steps,))] * 8,
        compiler_params=pltpu.CompilerParams(
            collective_id=collective_id, has_side_effects=True, vmem_limit_bytes=40 << 20
        ),
    )(part)


def contract_rows(left_side, right_side):
    return lax.dot_general(
        left_side, right_side, (((0,), (0,)), ((), ())), preferred_element_type=jnp.float32
    )


def contract_cols(left_side, right_side):
    return lax.dot_general(
        left_side, right_side, (((1,), (1,)), ((), ())), preferred_element_type=jnp.float32
    )


def expert_backward(routed_rows, routed_cots, w_gate, w_up, w_down):
    gate_pre = jnp.dot(routed_rows, w_gate, preferred_element_type=jnp.float32)
    up_pre = jnp.dot(routed_rows, w_up, preferred_element_type=jnp.float32)
    gate_clamped = jnp.minimum(gate_pre, CLAMP_LIMIT)
    up_clamped = jnp.clip(up_pre, -CLAMP_LIMIT, CLAMP_LIMIT)
    sigma = jax.nn.sigmoid(SLOPE_ALPHA * gate_clamped)
    gated = gate_clamped * sigma
    act = ((up_clamped + 1.0) * gated).astype(jnp.bfloat16)
    down_grad = contract_rows(act, routed_cots).astype(jnp.bfloat16)
    act_grad = contract_cols(routed_cots, w_down)
    inside = (up_pre > -CLAMP_LIMIT) & (up_pre < CLAMP_LIMIT)
    up_pre_grad = jnp.where(inside, act_grad * gated, 0.0).astype(jnp.bfloat16)
    slope = sigma + SLOPE_ALPHA * gate_clamped * sigma * (1.0 - sigma)
    gate_pre_grad = jnp.where(
        gate_pre < CLAMP_LIMIT, act_grad * (up_clamped + 1.0) * slope, 0.0
    ).astype(jnp.bfloat16)
    gate_grad = contract_rows(routed_rows, gate_pre_grad).astype(jnp.bfloat16)
    up_grad = contract_rows(routed_rows, up_pre_grad).astype(jnp.bfloat16)
    partial_value = contract_cols(gate_pre_grad, w_gate) + contract_cols(up_pre_grad, w_up)
    return (gate_grad, up_grad, down_grad, partial_value)


def local(
    grad_out,
    resid,
    norm_gain,
    routes,
    route_weights,
    gate_weight,
    up_weight,
    down_weight,
    proj_weight,
    conv_sum,
    conv_gain,
    conv_taps,
    conv_value,
    conv_gate,
):
    tok_rows, model_width = resid.shape
    sp_count = lax.axis_size("sp")
    tp_count = lax.axis_size("tp")
    capacity = 3 * tok_rows // sp_count
    col_count = model_width // tp_count
    resid_f = resid.astype(jnp.float32)
    inv_rms = lax.rsqrt(jnp.mean(resid_f * resid_f, axis=-1, keepdims=True) + 1e-06)
    normed = (resid_f * inv_rms * norm_gain).astype(jnp.bfloat16)
    my_sp = lax.axis_index("sp")
    away = (routes - my_sp) % sp_count
    steps_away = jnp.arange(sp_count, dtype=jnp.int32)
    named = away[:, :, None] == steps_away[None, None, :]
    chosen = jnp.any(named, axis=1)
    weight_of = jnp.sum(jnp.where(named, route_weights[:, :, None], 0.0), axis=1)
    token_ids = jnp.arange(tok_rows, dtype=jnp.int32)
    earlier = (token_ids[None, :] < token_ids[:, None]).astype(jnp.bfloat16)
    rank = jnp.dot(earlier, chosen.astype(jnp.bfloat16), preferred_element_type=jnp.float32)
    rank = jnp.where(chosen, rank, -1.0).astype(jnp.int32)
    slots = jnp.arange(capacity, dtype=jnp.int32)
    held = rank.T[:, None, :] == slots[None, :, None]
    slot_weight = jnp.sum(jnp.where(held, weight_of.T[:, None, :], 0.0), axis=2)
    pick = held.astype(jnp.bfloat16).reshape(sp_count * capacity, tok_rows)
    first_col = lax.axis_index("tp") * col_count
    normed_part = lax.dynamic_slice_in_dim(normed, first_col, col_count, 1)
    cots_part = lax.dynamic_slice_in_dim(grad_out, first_col, col_count, 1)
    slot_weight = slot_weight.reshape(-1, 1)
    send_rows = jnp.dot(pick, normed_part, preferred_element_type=jnp.float32).astype(jnp.bfloat16)
    send_cots = jnp.dot(pick, cots_part, preferred_element_type=jnp.float32)
    send_cots = (send_cots * slot_weight).astype(jnp.bfloat16)
    own_pick = pick[:capacity]
    own_rows = jnp.dot(own_pick, normed, preferred_element_type=jnp.float32).astype(jnp.bfloat16)
    own_cots = jnp.dot(own_pick, grad_out, preferred_element_type=jnp.float32)
    own_cots = (own_cots * slot_weight[:capacity]).astype(jnp.bfloat16)
    routed_rows, routed_cots = spread(
        (
            send_rows.reshape(sp_count, capacity, col_count),
            send_cots.reshape(sp_count, capacity, col_count),
        ),
        (own_rows, own_cots),
        None,
        True,
        False,
        0,
    )
    routed_rows = routed_rows.reshape(sp_count * capacity, model_width)
    routed_cots = routed_cots.reshape(sp_count * capacity, model_width)
    gate_grad, up_grad, down_grad, partial_value = expert_backward(
        routed_rows, routed_cots, gate_weight[0], up_weight[0], down_weight[0]
    )
    returned = combine(
        partial_value.reshape(sp_count, capacity, model_width).astype(jnp.bfloat16), 1
    ).reshape(sp_count * capacity, col_count)
    normed_part_grad = contract_rows(pick, returned).astype(jnp.bfloat16)
    channels = conv_sum.shape[1]
    summed = conv_sum.astype(jnp.float32).reshape(tok_rows, channels // GROUP, GROUP)
    centre = summed - jnp.mean(summed, axis=-1, keepdims=True)
    inv_std = lax.rsqrt(jnp.mean(centre * centre, axis=-1, keepdims=True) + 1e-05)
    grouped = centre * inv_std
    chan_normed = grouped.reshape(tok_rows, channels)
    pre_act = chan_normed * conv_gain
    sigma_conv = jax.nn.sigmoid(pre_act)
    conv_out = (pre_act * sigma_conv).astype(jnp.bfloat16)
    chunks = 4
    normed_grad, all_out = spread(
        (normed_part_grad.reshape(chunks, tok_rows // chunks, col_count),),
        None,
        conv_out,
        True,
        False,
        2,
    )
    normed_grad = normed_grad.reshape(tok_rows, model_width)
    feature_grad = normed_grad.astype(jnp.float32) * norm_gain
    cubed = inv_rms * inv_rms * inv_rms
    resid_grad = (
        grad_out.astype(jnp.float32)
        + inv_rms * feature_grad
        - resid_f * cubed * jnp.mean(resid_f * feature_grad, axis=-1, keepdims=True)
    ).astype(jnp.bfloat16)
    share = tok_rows // tp_count
    feat_rows = model_width // sp_count
    tokens_part = lax.dynamic_slice_in_dim(resid_grad, lax.axis_index("tp") * share, share, 0)
    by_feature = tokens_part.reshape(share, sp_count, feat_rows).transpose(1, 0, 2)
    own_features = lax.dynamic_slice_in_dim(resid_grad, my_sp * feat_rows, feat_rows, 1)
    (feature_cols,) = spread(
        (by_feature,), (own_features.reshape(tp_count, share, feat_rows),), None, False, True, 3
    )
    proj_grad = contract_rows(
        feature_cols.reshape(sp_count * tok_rows, feat_rows),
        all_out.reshape(sp_count * tok_rows, channels),
    )
    out_grad = jnp.dot(resid_grad, proj_weight, preferred_element_type=jnp.float32)
    normal_grad = (
        out_grad * sigma_conv * (1.0 + pre_act * (1.0 - sigma_conv)) * conv_gain
    ).reshape(tok_rows, channels // GROUP, GROUP)
    sum_grad = inv_std * (
        normal_grad
        - jnp.mean(normal_grad, axis=-1, keepdims=True)
        - grouped * jnp.mean(normal_grad * grouped, axis=-1, keepdims=True)
    )
    sum_grad = sum_grad.reshape(tok_rows, channels)
    following = passed_along(sum_grad[: CONV_K - 1], "sp", -1)
    extended = jnp.concatenate([sum_grad, following], axis=0)
    gated_grad = lax.conv_general_dilated(
        extended[None],
        conv_taps[::-1][:, None, :],
        (1,),
        ((0, 0),),
        dimension_numbers=("NWC", "WIO", "NWC"),
        feature_group_count=channels,
        precision=lax.Precision.HIGHEST,
    )[0]
    sigma_gate = jax.nn.sigmoid(conv_gate.astype(jnp.float32))
    value_grad = (gated_grad * sigma_gate).astype(jnp.bfloat16)
    gate_input_grad = (
        gated_grad * conv_value.astype(jnp.float32) * sigma_gate * (1.0 - sigma_gate)
    ).astype(jnp.bfloat16)
    return (gate_grad[None], up_grad[None], down_grad[None], proj_grad, value_grad, gate_input_grad)


def solution(mesh):
    in_specs = (
        P("sp", None),
        P("sp", None),
        P(),
        P("sp", None),
        P("sp", None),
        P("sp", None, "tp"),
        P("sp", None, "tp"),
        P("sp", "tp", None),
        P(None, "tp"),
        P("sp", "tp"),
        P("tp"),
        P(None, "tp"),
        P("sp", "tp"),
        P("sp", "tp"),
    )
    out_specs = (
        P("sp", None, "tp"),
        P("sp", None, "tp"),
        P("sp", "tp", None),
        P("sp", "tp"),
        P("sp", "tp"),
        P("sp", "tp"),
    )
    return jax.shard_map(local, mesh=mesh, in_specs=in_specs, out_specs=out_specs, check_vma=False)
```
